256 devices in a mesh: sp: 32 (over z, x), fs: 4 (over y), tp: 2 (over core).
Axes of the slice: x: 4, y: 4, z: 8, core: 2. Of those that a mesh axis runs over, the one named last changes fastest.
Arguments:
- inputs: bfloat16 [4, 8192, 2048], P('fs', ('sp', 'tp')), may hold values from -6 to 6
- norm_gain: float32 [2048], replicated, may hold values from 0.1 to 1.9
- w_glu_value: bfloat16 [2048, 1024], P(None, 'tp'), may hold values from -0.125 to 0.125
- w_glu_gate: bfloat16 [2048, 1024], P(None, 'tp'), may hold values from -0.125 to 0.125
- w_query_one: bfloat16 [2048, 512], P(None, 'tp'), may hold values from -2.5 to 2.5
- w_query_two: bfloat16 [2048, 512], P(None, 'tp'), may hold values from -2.5 to 2.5
- w_key_one: bfloat16 [2048, 512], P(None, 'tp'), may hold values from -2.5 to 2.5
- w_key_two: bfloat16 [2048, 512], P(None, 'tp'), may hold values from -2.5 to 2.5
- w_value: bfloat16 [2048, 1024], P(None, 'tp'), may hold values from -0.125 to 0.125
- conv_kernel: bfloat16 [31, 1024], P(None, 'tp'), may hold values from -1 to 1
- conv_gain: float32 [1024], P('tp'), may hold values from 0.1 to 1.9
- head_gain: float32 [128], replicated, may hold values from 0.1 to 1.9
- lambda_head: float32 [8], P('tp'), may hold values from 0.3 to 0.8
- w_out_conv: bfloat16 [1024, 2048], P('tp', 'fs'), may hold values from -0.125 to 0.125
- w_out_attn: bfloat16 [1024, 2048], P('tp', 'fs'), may hold values from -0.125 to 0.125
Outputs:
- mixed: bfloat16 [4, 8192, 2048], P('fs', ('sp', 'tp'))
- log_sums: float32 [4, 2, 8, 8192], P('fs', None, 'tp', 'sp')
The draws below stay inside these ranges and needn't reach their ends.
All inputs are finite; a program needn't handle non-finite values.
Results may differ from the reference program's by a relative error of at most 0.013.
Values may be sent and summed in bfloat16 or wider, within the bound.
No kernel may reach another device: no remote copies, remote signals or barrier semaphores. Data moves between devices by JAX's collectives and lax.ppermute only.
A program may use at most 128 MiB of HBM per device.

```python
import jax
import jax.numpy as jnp
from jax import lax

D = 2048
DC = 1024
H = 8
KVH = 8
HD = 64
VD = 128
CW = 31
SEG = 64
SEQ = 8192
BATCH = 4
DA = 1024


def query_key_pair(key, which):
    base_key = jax.random.fold_in(key, 7 + which)
    spread = (3.0 / D) ** 0.5
    key_weight = jax.random.normal(jax.random.fold_in(base_key, 1), (D, KVH * HD), jnp.float32) * spread
    query_weight = jax.random.normal(jax.random.fold_in(base_key, 2), (D, H * HD), jnp.float32) * spread
    return (jnp.clip(query_weight, -2.5, 2.5), jnp.clip(key_weight, -2.5, 2.5))


def draw_w_query_one(key, part):
    return query_key_pair(key, 1)[0].astype(jnp.bfloat16)


def draw_w_key_one(key, part):
    return query_key_pair(key, 1)[1].astype(jnp.bfloat16)


def draw_w_query_two(key, part):
    return query_key_pair(key, 2)[0].astype(jnp.bfloat16)


def draw_w_key_two(key, part):
    return query_key_pair(key, 2)[1].astype(jnp.bfloat16)


def steps_of(key, extent, pieces, low, high):
    gain, own = 1.0, jax.random.fold_in(key, 6)
    for dim, parts in pieces:
        heights = jnp.exp(jax.random.uniform(jax.random.fold_in(own, dim), (parts,), jnp.float32, low / len(pieces), high / len(pieces)))
        gain = gain * jnp.repeat(heights, extent[dim] // parts).reshape([-1 if axis == dim else 1 for axis in range(len(extent))])
    return gain


def gaussian(stream_key, shape, scale, most, cuts=(), held_as=jnp.bfloat16):
    loudness = steps_of(stream_key, shape, cuts, -0.22, 0.18) if cuts else 1.0
    result = jax.random.normal(stream_key, shape, jnp.float32) * scale * loudness
    return jnp.minimum(jnp.maximum(result, -most), most).astype(held_as)


def setup_inputs(seed: int = 0) -> dict:
    streams_of = jax.random.split(jax.random.key(seed), 16)
    inputs = gaussian(streams_of[0], (BATCH, SEQ, D), 1.0, 6.0, ((0, 4), (1, 64)))
    norm_gain = jnp.clip(1.0 + 0.18 * jax.random.normal(streams_of[1], (D,), jnp.float32), 0.1, 1.9)
    w_glu_value = gaussian(streams_of[2], (D, DC), D ** -0.5, 0.125, ((1, 2),))
    w_glu_gate = gaussian(streams_of[3], (D, DC), D ** -0.5, 0.125, ((1, 2),))
    w_query_one = draw_w_query_one(jax.random.fold_in(streams_of[15], 71), 0)
    w_query_two = draw_w_query_two(jax.random.fold_in(streams_of[15], 71), 0)
    w_key_one = draw_w_key_one(jax.random.fold_in(streams_of[15], 71), 0)
    w_key_two = draw_w_key_two(jax.random.fold_in(streams_of[15], 71), 0)
    w_value = gaussian(streams_of[8], (D, KVH * VD), D ** -0.5, 0.125, ((1, 2),))
    conv_kernel = gaussian(streams_of[9], (CW, DC), CW ** -0.5, 1.0, ((1, 2),))
    conv_gain = jnp.clip(1.0 + 0.18 * jax.random.normal(streams_of[10], (DC,), jnp.float32), 0.1, 1.9)
    head_gain = jnp.clip(1.0 + 0.18 * jax.random.normal(streams_of[11], (VD,), jnp.float32), 0.1, 1.9)
    lambda_head = jnp.clip(0.3 + 0.5 * jax.random.uniform(streams_of[12], (H,), jnp.float32) ** steps_of(streams_of[12], (H,), ((0, 2),), -0.2, 0.2), 0.3, 0.8)
    w_out_conv = gaussian(streams_of[13], (DC, D), (DC + DA) ** -0.5, 0.125, ((0, 2), (1, 4)))
    w_out_attn = gaussian(streams_of[14], (DA, D), (DC + DA) ** -0.5, 0.125, ((0, 2), (1, 4)))
    return dict(inputs=inputs, norm_gain=norm_gain, w_glu_value=w_glu_value, w_glu_gate=w_glu_gate, w_query_one=w_query_one, w_query_two=w_query_two, w_key_one=w_key_one, w_key_two=w_key_two, w_value=w_value, conv_kernel=conv_kernel, conv_gain=conv_gain, head_gain=head_gain, lambda_head=lambda_head, w_out_conv=w_out_conv, w_out_attn=w_out_attn)


NEG_FILL = -1e+30
EPSILON = 1e-05
HEAD_SCALE = 0.8

def one_sequence(seq_rows, norm_gain, w_glu_value, w_glu_gate, w_query_one, w_query_two, w_key_one, w_key_two, w_value, conv_kernel, conv_gain, head_gain, lambda_head, w_out_conv, w_out_attn):
    rows_f = seq_rows.astype(jnp.float32)
    normed = (rows_f * lax.rsqrt(lax.optimization_barrier(jnp.mean(rows_f * rows_f, axis=-1, keepdims=True)) + EPSILON) * norm_gain).astype(jnp.bfloat16)

    def project(weight):
        return jnp.dot(normed, weight, preferred_element_type=jnp.float32).astype(jnp.bfloat16)
    glu_value = project(w_glu_value)
    glu_gate = project(w_glu_gate)
    query_one = project(w_query_one)
    query_two = project(w_query_two)
    key_one = project(w_key_one)
    key_two = project(w_key_two)
    values = project(w_value)
    gated = (glu_value.astype(jnp.float32) * jax.nn.sigmoid(glu_gate.astype(jnp.float32))).astype(jnp.bfloat16)
    extended = jnp.concatenate([jnp.zeros((CW - 1, DC), jnp.bfloat16), gated], axis=0).astype(jnp.float32)
    kernel_f = conv_kernel.astype(jnp.float32)
    convolved = jnp.zeros((SEQ, DC), jnp.float32)
    for tap_index in range(CW):
        convolved = convolved + kernel_f[tap_index][None, :] * extended[tap_index:tap_index + SEQ]
    row_mean = lax.optimization_barrier(jnp.mean(convolved, axis=-1, keepdims=True))
    row_square = lax.optimization_barrier(jnp.mean(convolved * convolved, axis=-1, keepdims=True))
    conv_out = jax.nn.silu((convolved - row_mean) * lax.rsqrt(row_square - row_mean * row_mean + EPSILON) * conv_gain).astype(jnp.bfloat16)
    group = H // KVH
    query_one_r = query_one.reshape(SEQ, KVH, group, HD).astype(jnp.float32)
    query_two_r = query_two.reshape(SEQ, KVH, group, HD).astype(jnp.float32)
    key_one_r = key_one.reshape(SEQ, KVH, HD).astype(jnp.float32)
    key_two_r = key_two.reshape(SEQ, KVH, HD).astype(jnp.float32)
    values_r = values.reshape(SEQ, KVH, VD).astype(jnp.float32)
    lambda_r = lambda_head.reshape(KVH, group)
    score_scale = HD ** (-0.5)
    block_rows = min(512, SEQ)
    attn_blocks = []
    log_blocks = []
    for block_start in range(0, SEQ, block_rows):
        block_end = min(block_start + block_rows, SEQ)
        query_pos = jnp.arange(block_start, block_end, dtype=jnp.int32)
        key_pos = jnp.arange(0, block_end, dtype=jnp.int32)
        allowed = ((key_pos // SEG)[None, :] <= (query_pos // SEG)[:, None])[:, None, None, :]
        pooled_list = []
        log_list = []
        for queries, key_rows in ((query_one_r, key_one_r), (query_two_r, key_two_r)):
            scores = jnp.einsum('tgrd,kgd->tgrk', queries[block_start:block_end], key_rows[:block_end]) * score_scale
            scores = jnp.where(allowed, scores, NEG_FILL)
            row_max = lax.optimization_barrier(jnp.max(scores, axis=-1))
            weights = jnp.where(allowed, jnp.exp(scores - row_max[..., None]), 0.0)
            weight_sum = lax.optimization_barrier(jnp.sum(weights, axis=-1))
            log_list.append(row_max + jnp.log(weight_sum))
            pooled = jnp.einsum('tgrk,kgv->tgrv', weights.astype(jnp.bfloat16).astype(jnp.float32), values_r[:block_end])
            pooled_list.append(pooled / weight_sum[..., None])
        head_out = pooled_list[0] - lambda_r[None, :, :, None] * pooled_list[1]
        head_out = head_out * lax.rsqrt(lax.optimization_barrier(jnp.mean(head_out * head_out, axis=-1, keepdims=True)) + EPSILON) * head_gain * HEAD_SCALE
        attn_blocks.append(head_out.astype(jnp.bfloat16).reshape(block_end - block_start, H * VD))
        log_blocks.append(jnp.stack(log_list, axis=0).reshape(2, block_end - block_start, H))
    attn_out = jnp.concatenate(attn_blocks, axis=0)
    log_sums = jnp.transpose(jnp.concatenate(log_blocks, axis=1), (0, 2, 1))
    mixed = jnp.dot(conv_out, w_out_conv, preferred_element_type=jnp.float32) + jnp.dot(attn_out, w_out_attn, preferred_element_type=jnp.float32)
    return (mixed.astype(jnp.bfloat16), log_sums)

def reference(inputs, norm_gain, w_glu_value, w_glu_gate, w_query_one, w_query_two, w_key_one, w_key_two, w_value, conv_kernel, conv_gain, head_gain, lambda_head, w_out_conv, w_out_attn):

    def per_sequence(seq_rows):
        return one_sequence(seq_rows, norm_gain, w_glu_value, w_glu_gate, w_query_one, w_query_two, w_key_one, w_key_two, w_value, conv_kernel, conv_gain, head_gain, lambda_head, w_out_conv, w_out_attn)
    mixed, log_sums = lax.map(per_sequence, inputs)
    return (mixed, log_sums)
```

```python
import functools

import jax
import jax.numpy as jnp
from jax import lax
from jax.experimental import pallas as pl
from jax.experimental.pallas import tpu as pltpu
from jax.sharding import Mesh, PartitionSpec as P

D = 2048
DC = 1024
HD = 64
VD = 128
CW = 31
SEG = 64
NZ, NX, NF, NT = 8, 4, 4, 2
BLOCK = 256
HALF = 128

NEG_FILL = -1e30
EPSILON = 1e-05
HEAD_SCALE = 0.8
LOG2E = 1.4426950408889634


SWAP = [(0, 1), (1, 0)]
BF = jnp.bfloat16
F32 = jnp.float32


def head_route(step):
    return [
        (z * NT + t, (4 * t + (z + step) % 4) * NT + z // 4) for z in range(NZ) for t in range(NT)
    ]


def ring(count, step):
    return [(i, (i + step) % count) for i in range(count)]


def proj_kernel(pos, own, peer, wk1, wk2, wq1, wq2, wv, x_out, m0, m1, m2, m3, packed):
    step = pl.program_id(0)
    z, t = pos[0], pos[2]

    @pl.when(step == 0)
    def _():
        x_out[pl.ds(pl.multiple_of(t * HALF, HALF), HALF), :] = own[...]
        x_out[pl.ds(pl.multiple_of((1 - t) * HALF, HALF), HALF), :] = peer[...]

    rows = x_out[...]

    def dot(w):
        return jnp.dot(rows, w[...], preferred_element_type=F32).astype(BF).astype(F32)

    k1, k2, v = dot(wk1), dot(wk2), dot(wv)
    q1, q2 = dot(wq1), dot(wq2)
    low = lax.broadcasted_iota(jnp.int32, (BLOCK, 2 * HD), 1) < HD

    def pair(a, b, e):
        if e == 0:
            return jnp.where(low, a, pltpu.roll(b, HD, 1))
        return jnp.where(low, pltpu.roll(a, HD, 1), b)

    for e in range(2):
        head = 2 * step + e
        packed[head, :, 0:128] = pair(k1, k2, e).astype(BF)
        q = pair(q1, q2, e) * (HD**-0.5)
        ve = v[:, e * VD : (e + 1) * VD]
        for half in range(2):
            sl = slice(half * HALF, (half + 1) * HALF)
            packed[head, sl, 128:256] = ve[sl].T.astype(BF)
            packed[head, sl, 256:384] = q[sl].T.astype(BF)

    @pl.when(step == 1)
    def _():
        for j, out in enumerate((m0, m1, m2, m3)):
            out[...] = packed[(z + j) % 4]


def project(pos, own, peer, wk1, wk2, wq1, wq2, wv):
    full = lambda shape: pl.BlockSpec(shape, lambda i, *_: (0,) * len(shape))
    wide = lambda cols: pl.BlockSpec((D, cols), lambda i, *_: (0, i))
    return pl.pallas_call(
        proj_kernel,
        grid_spec=pltpu.PrefetchScalarGridSpec(
            num_scalar_prefetch=1,
            grid=(2,),
            in_specs=[full((HALF, D)), full((HALF, D))] + [wide(128)] * 4 + [wide(256)],
            out_specs=[full((BLOCK, D))] + [full((BLOCK, 384))] * 4,
            scratch_shapes=[pltpu.VMEM((4, BLOCK, 384), BF)],
        ),
        out_shape=[jax.ShapeDtypeStruct((BLOCK, D), BF)]
        + [jax.ShapeDtypeStruct((BLOCK, 384), BF)] * 4,
        compiler_params=pltpu.CompilerParams(dimension_semantics=("arbitrary",)),
        cost_estimate=pl.CostEstimate(
            flops=2 * BLOCK * D * 1536, transcendentals=0, bytes_accessed=8 * 2**20
        ),
        name="project",
    )(pos, own, peer, wk1, wk2, wq1, wq2, wv)


def attend_shard(pos, x2, kv_a, kv_b, kv_s, q_s, m_s, l_s, acc_s):
    z, x, t = pos[0], pos[1], pos[2]
    for j in range(4):
        zz = (z + 4 - j) % 4
        kv_s[4 * t + zz] = kv_a[j]
        kv_s[4 * (1 - t) + zz] = kv_b[j]
    key_seg = lax.broadcasted_iota(jnp.int32, (BLOCK, 256), 0) // SEG
    query_seg = (lax.broadcasted_iota(jnp.int32, (BLOCK, 256), 1) % HALF) // SEG
    allowed = key_seg - query_seg <= 2 * t + 8 * (x - x2)

    def scores(zq):
        q = q_s[zq]
        parts = []
        for z2 in range(zq + 1):
            s = jnp.dot(kv_s[z2, :, 0:128], q, preferred_element_type=F32)
            if z2 == zq:
                s = jnp.where(allowed, s, NEG_FILL)
            parts.append(s)
        return parts

    def absorb(zq, parts):
        m_old = m_s[zq]
        top = parts[0]
        for s in parts[1:]:
            top = jnp.maximum(top, s)
        m_new = jnp.maximum(m_old, jnp.max(top, axis=0, keepdims=True))
        factor = jnp.exp2((m_old - m_new) * LOG2E)
        total = None
        pooled = None
        for z2, s in enumerate(parts):
            w = jnp.exp2((s - m_new) * LOG2E)
            total = w if total is None else total + w
            vt = jnp.concatenate([kv_s[z2, 0:128, 128:256], kv_s[z2, 128:256, 128:256]], axis=1)
            o = jnp.dot(vt, w.astype(BF), preferred_element_type=F32)
            pooled = o if pooled is None else pooled + o
        m_s[zq] = m_new
        l_s[zq] = l_s[zq] * factor + jnp.sum(total, axis=0, keepdims=True)
        acc_s[zq] = acc_s[zq] * factor + pooled

    parts = scores(0)
    for zq in range(NZ):
        following = scores(zq + 1) if zq + 1 < NZ else None
        absorb(zq, parts)
        parts = following


def first_kernel(pos, q_own, q_peer, kv_a, kv_b, q_s, m_s, l_s, acc_s, kv_s):
    z, x, t = pos[0], pos[1], pos[2]
    upper = lax.broadcasted_iota(jnp.int32, (128, HALF), 0) < HD
    for j in range(4):
        zz = (z + 4 - j) % 4
        for base, q in ((4 * t, q_own), (4 * (1 - t), q_peer)):
            qt = q[j].astype(F32)
            q_s[base + zz, :, 0:HALF] = jnp.where(upper, qt, 0.0).astype(BF)
            q_s[base + zz, :, HALF:256] = jnp.where(upper, 0.0, qt).astype(BF)
    m_s[...] = jnp.full(m_s.shape, NEG_FILL, F32)
    l_s[...] = jnp.zeros(l_s.shape, F32)
    acc_s[...] = jnp.zeros(acc_s.shape, F32)
    attend_shard(pos, x, kv_a, kv_b, kv_s, q_s, m_s, l_s, acc_s)


def middle_kernel(pos, q_s, m_i, l_i, acc_i, kv_a, kv_b, m_s, l_s, acc_s, kv_s, *, step):
    m_s[...] = m_i[...]
    l_s[...] = l_i[...]
    acc_s[...] = acc_i[...]
    x2 = (pos[1] + step) % 4
    attend_shard(pos, x2, kv_a, kv_b, kv_s, q_s, m_s, l_s, acc_s)


def last_kernel(
    pos, lam, gain, q_s, m_i, l_i, acc_i, kv_a, kv_b, out, m_s, l_s, acc_s, kv_s, *, step
):
    middle_kernel(pos, q_s, m_i, l_i, acc_i, kv_a, kv_b, m_s, l_s, acc_s, kv_s, step=step)
    lam_h = lam[pos[0]]
    for zq in range(NZ):
        denominator = l_s[zq]
        scaled = acc_s[zq] / denominator
        head = scaled[:, 0:HALF] - lam_h * scaled[:, HALF:256]
        square = jnp.mean(head * head, axis=0, keepdims=True)
        head = head * lax.rsqrt(square + EPSILON) * gain[...] * HEAD_SCALE
        out[zq, 0:HALF, :] = head.T.astype(BF)
        logs = m_s[zq] + jnp.log(denominator)
        high = logs.astype(BF).astype(F32)
        rest = logs - high
        tail = jnp.concatenate(
            [
                high[:, 0:HALF],
                high[:, HALF:256],
                rest[:, 0:HALF],
                rest[:, HALF:256],
                jnp.zeros((4, HALF), F32),
            ],
            axis=0,
        )
        out[zq, HALF : HALF + 8, :] = tail.astype(BF)


KV_SHARD = (4, BLOCK, 256)
STATE = [
    jax.ShapeDtypeStruct((NZ, 1, 256), F32),
    jax.ShapeDtypeStruct((NZ, 1, 256), F32),
    jax.ShapeDtypeStruct((NZ, 128, 256), F32),
]
SMEM = pl.BlockSpec(memory_space=pltpu.SMEM)
VMEM = pl.BlockSpec(memory_space=pltpu.VMEM)
ATTEND_COST = pl.CostEstimate(
    flops=2 * 36 * BLOCK * 256 * 256, transcendentals=36 * BLOCK * 256, bytes_accessed=4 * 2**20
)


def attend_first(pos, q_own, q_peer, kv_a, kv_b):
    return pl.pallas_call(
        first_kernel,
        in_specs=[SMEM] + [VMEM] * 4,
        out_specs=[VMEM] * 4,
        out_shape=[jax.ShapeDtypeStruct((NZ, 128, 256), BF)] + STATE,
        scratch_shapes=[pltpu.VMEM((NZ, BLOCK, 256), BF)],
        cost_estimate=ATTEND_COST,
        name="attend_first",
    )(pos, q_own, q_peer, kv_a, kv_b)


def attend_middle(pos, q_s, state, kv_a, kv_b, step):
    return pl.pallas_call(
        functools.partial(middle_kernel, step=step),
        in_specs=[SMEM] + [VMEM] * 6,
        out_specs=[VMEM] * 3,
        out_shape=STATE,
        scratch_shapes=[pltpu.VMEM((NZ, BLOCK, 256), BF)],
        cost_estimate=ATTEND_COST,
        name="attend_middle",
    )(pos, q_s, *state, kv_a, kv_b)


def attend_last(pos, lam, gain, q_s, state, kv_a, kv_b, step):
    return pl.pallas_call(
        functools.partial(last_kernel, step=step),
        in_specs=[SMEM, SMEM] + [VMEM] * 7,
        out_specs=VMEM,
        out_shape=jax.ShapeDtypeStruct((NZ, HALF + 8, 128), BF),
        scratch_shapes=[
            pltpu.VMEM((NZ, 1, 256), F32),
            pltpu.VMEM((NZ, 1, 256), F32),
            pltpu.VMEM((NZ, 128, 256), F32),
            pltpu.VMEM((NZ, BLOCK, 256), BF),
        ],
        cost_estimate=ATTEND_COST,
        name="attend_last",
    )(pos, lam, gain, q_s, *state, kv_a, kv_b)


def conv_mix_kernel(c_own, c_peer, w0, w1, w2, w3, v0, v1, v2, v3, out):
    for d, (w, v) in enumerate(((w0, v0), (w1, v1), (w2, v2), (w3, v3))):
        out[d] = jnp.dot(c_own[...], w[0:512, :], preferred_element_type=F32) + jnp.dot(
            c_peer[...], v[0:512, :], preferred_element_type=F32
        )


def final_kernel(pos, heads, part, w0, w1, w2, w3, v0, v1, v2, v3, out):
    z, y, t = pos[0], pos[3], pos[2]

    def side(base):
        return jnp.concatenate([heads[base + i, 0:HALF, :] for i in range(4)], axis=1)

    a_own = side(4 * t)
    a_peer = side(4 * (1 - t))
    for d, (w, v) in enumerate(((w0, v0), (w1, v1), (w2, v2), (w3, v3))):
        mixed = (
            part[d]
            + jnp.dot(a_own, w[...], preferred_element_type=F32)
            + jnp.dot(a_peer, v[...], preferred_element_type=F32)
        )
        column = ((y + 4 - d) % 4) * 512
        out[:, pl.ds(pl.multiple_of(column, 512), 512)] = mixed.astype(BF)


def conv_mix(c_own, c_peer, ws):
    block = pl.BlockSpec((512, 512), lambda i: (0, 0))
    row = pl.BlockSpec((HALF, 512), lambda i: (0, 0))
    return pl.pallas_call(
        conv_mix_kernel,
        grid=(1,),
        in_specs=[row] * 2 + [block] * 8,
        out_specs=pl.BlockSpec((4, HALF, 512), lambda i: (0, 0, 0)),
        out_shape=jax.ShapeDtypeStruct((4, HALF, 512), F32),
        cost_estimate=pl.CostEstimate(
            flops=2 * HALF * 1024 * 2048, transcendentals=0, bytes_accessed=6 * 2**20
        ),
        name="conv_mix",
    )(c_own, c_peer, *ws)


def final_mix(pos, heads, part, ws):
    block = pl.BlockSpec((512, 512), lambda i, *_: (1, 0))
    return pl.pallas_call(
        final_kernel,
        grid_spec=pltpu.PrefetchScalarGridSpec(
            num_scalar_prefetch=1,
            grid=(1,),
            in_specs=[
                pl.BlockSpec((8, HALF + 8, 128), lambda i, *_: (0, 0, 0)),
                pl.BlockSpec((4, HALF, 512), lambda i, *_: (0, 0, 0)),
            ]
            + [block] * 8,
            out_specs=pl.BlockSpec((HALF, D), lambda i, *_: (0, 0)),
        ),
        out_shape=jax.ShapeDtypeStruct((HALF, D), BF),
        cost_estimate=pl.CostEstimate(
            flops=2 * HALF * 1024 * 2048, transcendentals=0, bytes_accessed=6 * 2**20
        ),
        name="final_mix",
    )(pos, heads, part, *ws)


def body(
    inputs,
    norm_gain,
    w_glu_value,
    w_glu_gate,
    w_query_one,
    w_query_two,
    w_key_one,
    w_key_two,
    w_value,
    conv_kernel,
    conv_gain,
    head_gain,
    lambda_head,
    w_out_conv,
    w_out_attn,
):
    z, x, y, t = (lax.axis_index(a) for a in ("z", "x", "fs", "tp"))
    pos = jnp.stack([z, x, t, y]).astype(jnp.int32)

    def swap(value):
        return lax.ppermute(value, "tp", SWAP)

    rows_f = inputs[0].astype(F32)
    own = (
        rows_f * lax.rsqrt(jnp.mean(rows_f * rows_f, axis=-1, keepdims=True) + EPSILON) * norm_gain
    ).astype(BF)
    peer = swap(own)
    lambda_peer = swap(lambda_head)
    lambda_all = jnp.where(
        t == 0,
        jnp.concatenate([lambda_head, lambda_peer]),
        jnp.concatenate([lambda_peer, lambda_head]),
    )

    w_own = jnp.concatenate([w_out_conv, w_out_attn], axis=0)
    w_sides = [w_own] + [lax.ppermute(w_own, "fs", ring(NF, d)) for d in (1, 2, 3)]

    normed, *messages = project(
        pos, own, peer, w_key_one, w_key_two, w_query_one, w_query_two, w_value
    )

    arrived = [lax.ppermute(m, ("z", "tp"), head_route(j)) for j, m in enumerate(messages)]
    kv = jnp.stack([m[:, 0:256] for m in arrived])
    queries = jnp.stack([m[:, 256:384] for m in arrived]).reshape(4, 2, HALF, 128)
    q_own = lax.dynamic_index_in_dim(queries, t, 1, keepdims=False)
    q_peer = swap(lax.dynamic_index_in_dim(queries, 1 - t, 1, keepdims=False))

    shards = {0: kv}
    for step in (1, 3, 2):
        shards[(-step) % 4] = lax.ppermute(kv, "x", ring(NX, step))
    swapped = {k: swap(v) for k, v in shards.items()}

    glu_value = jnp.dot(normed, w_glu_value, preferred_element_type=F32).astype(BF)
    glu_gate = jnp.dot(normed, w_glu_gate, preferred_element_type=F32).astype(BF)
    gated = (glu_value.astype(F32) * jax.nn.sigmoid(glu_gate.astype(F32))).astype(BF)
    count = NZ * NX
    earlier = lax.ppermute(
        gated[BLOCK - (CW - 1) :], ("z", "x"), [(i, i + 1) for i in range(count - 1)]
    )
    extended = jnp.concatenate([earlier, gated], axis=0).astype(F32)
    kernel_f = conv_kernel.astype(F32)
    convolved = jnp.zeros((BLOCK, 512), F32)
    for tap in range(CW):
        convolved = convolved + kernel_f[tap][None, :] * extended[tap : tap + BLOCK]
    sums = jnp.stack([jnp.sum(convolved, axis=-1), jnp.sum(convolved * convolved, axis=-1)])
    sums = sums + swap(sums)
    row_mean = (sums[0] / DC)[:, None]
    row_square = (sums[1] / DC)[:, None]
    conv_out = jax.nn.silu(
        (convolved - row_mean) * lax.rsqrt(row_square - row_mean * row_mean + EPSILON) * conv_gain
    ).astype(BF)
    conv_halves = conv_out.reshape(2, HALF, 512)
    conv_own = lax.dynamic_index_in_dim(conv_halves, t, 0, keepdims=False)
    conv_peer = swap(lax.dynamic_index_in_dim(conv_halves, 1 - t, 0, keepdims=False))
    w_all = w_sides + [swap(w) for w in w_sides]
    part = conv_mix(conv_own, conv_peer, w_all)

    q_s, *state = attend_first(pos, q_own, q_peer, shards[0], swapped[0])
    state = attend_middle(pos, q_s, state, shards[3], swapped[3], 3)
    state = attend_middle(pos, q_s, state, shards[1], swapped[1], 1)
    gain = head_gain.reshape(VD, 1)
    returned = attend_last(pos, lambda_all, gain, q_s, state, shards[2], swapped[2], 2)

    heads = lax.all_to_all(returned, "z", 0, 0, tiled=True)
    mixed = final_mix(pos, heads, part, w_all)

    tails = heads[:, HALF : HALF + 4, :].astype(F32)
    logs = (tails[:, 0:2] + tails[:, 2:4]).reshape(2, 4, 2, HALF)
    logs_own = lax.dynamic_index_in_dim(logs, t, 0, keepdims=False)
    logs_peer = swap(lax.dynamic_index_in_dim(logs, 1 - t, 0, keepdims=False))
    first = jnp.where(t == 0, logs_own, logs_peer)
    second = jnp.where(t == 0, logs_peer, logs_own)
    log_sums = jnp.transpose(jnp.concatenate([first, second], axis=-1), (1, 0, 2))
    return (mixed[None], log_sums[None])


def solution(mesh):
    grid = Mesh(mesh.devices.reshape(NZ, NX, NF, NT), ("z", "x", "fs", "tp"))
    weight = P(None, "tp")
    return jax.shard_map(
        body,
        mesh=grid,
        in_specs=(
            P("fs", ("z", "x", "tp"), None),
            P(),
            weight,
            weight,
            weight,
            weight,
            weight,
            weight,
            weight,
            weight,
            P("tp"),
            P(),
            P("tp"),
            P("tp", "fs"),
            P("tp", "fs"),
        ),
        out_specs=(P("fs", ("z", "x", "tp"), None), P("fs", None, "tp", ("z", "x"))),
        check_vma=False,
    )
```

```python
import functools

import jax
import jax.numpy as jnp
from jax import lax
from jax.experimental import pallas as pl
from jax.experimental.pallas import tpu as pltpu
from jax.sharding import Mesh, PartitionSpec as P


D = 2048
DC = 1024
HD = 64
VD = 128
CW = 31
SEG = 64
NZ, NX, NF, NT = 8, 4, 4, 2
BLOCK = 256
HALF = 128

NEG_FILL = -1e30
EPSILON = 1e-05
HEAD_SCALE = 0.8
LOG2E = 1.4426950408889634
LN2 = 0.6931471805599453


SWAP = [(0, 1), (1, 0)]
BF = jnp.bfloat16
F32 = jnp.float32


def head_route(step):
    return [
        (z * NT + t, (4 * t + (z + step) % 4) * NT + z // 4) for z in range(NZ) for t in range(NT)
    ]


def ring(count, step):
    return [(i, (i + step) % count) for i in range(count)]


def proj_kernel(
    own, peer, gain, wk1, wk2, wq1, wq2, wv, x_out, m0, m1, m2, m3, hk1, hk2, hq1, hq2, hv, packed, sems
):
    z, _, t = places()
    copies = [
        pltpu.make_async_copy(w, held, sems.at[i])
        for i, (w, held) in enumerate(
            ((wk1, hk1), (wk2, hk2), (wv, hv), (wq1, hq1), (wq2, hq2))
        )
    ]
    for copy in copies:
        copy.start()
    for place, rows in ((t, own), (1 - t, peer)):
        r = rows[...].astype(F32)
        scale = lax.rsqrt(jnp.mean(r * r, axis=-1, keepdims=True) + EPSILON)
        x_out[pl.ds(pl.multiple_of(place * HALF, HALF), HALF), :] = (r * scale * gain[...]).astype(
            BF
        )
    low = lax.broadcasted_iota(jnp.int32, (BLOCK, 2 * HD), 1) < HD

    def dot(held):
        return jnp.dot(x_out[...], held[...], preferred_element_type=F32).astype(BF).astype(F32)

    def both(a, b, head):
        pair = (head // 2) * 128
        a, b = a[:, pair : pair + 128], b[:, pair : pair + 128]
        if head % 2 == 0:
            return jnp.where(low, a, pltpu.roll(b, HD, 1))
        return jnp.where(low, pltpu.roll(a, HD, 1), b)

    def turned(value, head, column):
        for half in range(2):
            sl = slice(half * HALF, (half + 1) * HALF)
            packed[head, sl, column : column + 128] = value[sl].T.astype(BF)

    copies[0].wait()
    k1 = dot(hk1)
    copies[1].wait()
    k2 = dot(hk2)
    for head in range(4):
        packed[head, :, 0:128] = both(k1, k2, head).astype(BF)
    copies[2].wait()
    v = dot(hv)
    for head in range(4):
        turned(v[:, head * VD : (head + 1) * VD], head, 128)
    copies[3].wait()
    q1 = dot(hq1)
    copies[4].wait()
    q2 = dot(hq2)
    for head in range(4):
        turned(both(q1, q2, head) * (HD**-0.5), head, 256)
    for j, out in enumerate((m0, m1, m2, m3)):
        out[...] = packed[(z + j) % 4]


def project(own, peer, gain, wk1, wk2, wq1, wq2, wv):
    return pl.pallas_call(
        proj_kernel,
        in_specs=[VMEM] * 3 + [ANY] * 5,
        out_specs=[VMEM] * 5,
        out_shape=[jax.ShapeDtypeStruct((BLOCK, D), BF)]
        + [jax.ShapeDtypeStruct((BLOCK, 384), BF)] * 4,
        scratch_shapes=[pltpu.VMEM((D, 256), BF)] * 4
        + [
            pltpu.VMEM((D, 512), BF),
            pltpu.VMEM((4, BLOCK, 384), BF),
            pltpu.SemaphoreType.DMA((5,)),
        ],
        cost_estimate=pl.CostEstimate(
            flops=2 * BLOCK * D * 1536, transcendentals=0, bytes_accessed=8 * 2**20
        ),
        name="project",
    )(own, peer, gain, wk1, wk2, wq1, wq2, wv)


SMEM = pl.BlockSpec(memory_space=pltpu.SMEM)
VMEM = pl.BlockSpec(memory_space=pltpu.VMEM)
ANY = pl.BlockSpec(memory_space=pl.ANY)


def places():
    return tuple(lax.axis_index(a) for a in ("z", "x", "tp"))


def shard_copies(kv_a, kv_b, kv_s, sems, first=0):
    z, _, t = places()
    copies = []
    for j in range(kv_a.shape[0]):
        zz = (z + 4 - first - j) % 4
        for slot, kv in ((4 * t + zz, kv_a), (4 * (1 - t) + zz, kv_b)):
            sem = sems.at[2 * (first + j) + (kv is kv_b)]
            copies.append(pltpu.make_async_copy(kv.at[j], kv_s.at[slot], sem))
    return copies


def start(copies):
    for copy in copies:
        copy.start()


def wait(copies):
    for copy in copies:
        copy.wait()


def attend_shard(x2, kv_s, q_s, m_s, l_s, acc_s, before=None, after=None):
    _, x, t = places()
    key_seg = lax.broadcasted_iota(jnp.int32, (BLOCK, 256), 0) // SEG
    query_seg = (lax.broadcasted_iota(jnp.int32, (BLOCK, 256), 1) % HALF) // SEG
    allowed = key_seg - query_seg <= 2 * t + 8 * (x - x2)

    ones = jnp.ones((8, BLOCK), BF)

    def scores(zq):
        q = q_s[zq]
        parts = []
        for z2 in range(zq + 1):
            k = kv_s[z2, :, 0:128]
            s = jnp.dot(jnp.concatenate([k, k], axis=1), q, preferred_element_type=F32)
            if z2 == zq:
                s = jnp.where(allowed, s, NEG_FILL)
            parts.append(s)
        return parts

    def absorb(zq, parts):
        m_old = m_s[zq]
        top = None
        for s in parts:
            best = jnp.max(s.reshape(BLOCK // 8, 8, 256), axis=0)
            top = best if top is None else jnp.maximum(top, best)
        m_new = jnp.maximum(m_old, jnp.max(top, axis=0, keepdims=True))
        factor = jnp.exp2(m_old - m_new)
        weights = []
        values = []
        for z2, s in enumerate(parts):
            weights.append(jnp.exp2(s - m_new).astype(BF))
            vt = jnp.concatenate([kv_s[z2, 0:128, 128:256], kv_s[z2, 128:256, 128:256]], axis=1)
            values.append(jnp.concatenate([vt, ones], axis=0))
        pooled = jnp.dot(
            jnp.concatenate(values, axis=1),
            jnp.concatenate(weights, axis=0),
            preferred_element_type=F32,
        )
        m_s[zq] = m_new
        l_s[zq] = l_s[zq] * factor + pooled[128:129]
        acc_s[zq] = acc_s[zq] * factor + pooled[0:128]

    parts = scores(0)
    if before is not None:
        before()
    for zq in range(NZ):
        following = scores(zq + 1) if zq + 1 < NZ else None
        absorb(zq, parts)
        if after is not None:
            after(zq)
        parts = following


def state_copies(state, held, sems, inward):
    pairs = zip(state, held)
    return [
        pltpu.make_async_copy(*((a, b) if inward else (b, a)), sems.at[i])
        for i, (a, b) in enumerate(pairs)
    ]


def chunk_copy(acc_s, acc, sems, zq):
    return pltpu.make_async_copy(acc_s.at[zq], acc.at[zq], sems.at[zq])


def first_kernel(
    q_own, q_peer, kv_a, kv_b, q_out, m_out, l_out, acc_out, qt_s, q_s, m_s, l_s, acc_s, kv_s, sems, out_sems, aux
):
    z, x, t = places()
    queries = [
        pltpu.make_async_copy(q_own, qt_s.at[0], aux.at[0]),
        pltpu.make_async_copy(q_peer, qt_s.at[1], aux.at[1]),
    ]
    shard = shard_copies(kv_a, kv_b, kv_s, sems)
    start(queries)
    start(shard)
    m_s[...] = jnp.full(m_s.shape, NEG_FILL, F32)
    l_s[...] = jnp.zeros(l_s.shape, F32)
    acc_s[...] = jnp.zeros(acc_s.shape, F32)
    wait(queries)
    upper = lax.broadcasted_iota(jnp.int32, (128, HALF), 0) < HD
    for j in range(4):
        zz = (z + 4 - j) % 4
        for side, base in ((0, 4 * t), (1, 4 * (1 - t))):
            qt = qt_s[side, j].astype(F32) * LOG2E
            high = qt.astype(BF).astype(F32)
            for row, part in ((0, high), (128, qt - high)):
                q_s[base + zz, row : row + 128, 0:HALF] = jnp.where(upper, part, 0.0).astype(BF)
                q_s[base + zz, row : row + 128, HALF:256] = jnp.where(upper, 0.0, part).astype(BF)
    spread = pltpu.make_async_copy(q_s, q_out, aux.at[2])
    spread.start()
    wait(shard)
    chunks = [chunk_copy(acc_s, acc_out, out_sems, zq) for zq in range(NZ)]
    attend_shard(x, kv_s, q_s, m_s, l_s, acc_s, after=lambda zq: chunks[zq].start())
    ends = state_copies((m_out, l_out), (m_s, l_s), aux, False)
    start(ends)
    spread.wait()
    wait(chunks)
    wait(ends)


def middle_kernel(
    q_i,
    m_i,
    l_i,
    acc_i,
    kv_a,
    kv_b,
    kv_c,
    kv_d,
    m_out,
    l_out,
    acc_out,
    q_s,
    m_s,
    l_s,
    acc_s,
    kv_s,
    sems,
    out_sems,
    aux,
    *,
    steps,
):
    _, x, _ = places()
    queries = pltpu.make_async_copy(q_i, q_s, aux.at[3])
    first = shard_copies(kv_a, kv_b, kv_s.at[0], sems.at[0])
    state = state_copies((m_i, l_i, acc_i), (m_s, l_s, acc_s), aux, True)
    second = shard_copies(kv_c, kv_d, kv_s.at[1], sems.at[1])
    queries.start()
    start(first)
    start(state)
    start(second)
    queries.wait()
    wait(first)
    chunks = [chunk_copy(acc_s, acc_out, out_sems, zq) for zq in range(NZ)]

    @pl.loop(0, 2)
    def _(i):
        @pl.when(i == 0)
        def _():
            wait(state)

        @pl.when(i == 1)
        def _():
            wait(second)

        def after(zq):
            @pl.when(i == 1)
            def _():
                chunks[zq].start()

        x2 = (x + jnp.where(i == 0, steps[0], steps[1])) % 4
        attend_shard(x2, kv_s.at[i], q_s, m_s, l_s, acc_s, after=after)

    ends = state_copies((m_out, l_out), (m_s, l_s), aux, False)
    start(ends)
    wait(chunks)
    wait(ends)


def last_kernel(
    lam_a, lam_b, gain, q_s, m_i, l_i, acc_i, kv_a, kv_b, out, m_s, l_s, acc_s, kv_s, *, step
):
    z, x, t = places()
    m_s[...] = m_i[...]
    l_s[...] = l_i[...]
    acc_s[...] = acc_i[...]
    for j in range(4):
        zz = (z + 4 - j) % 4
        kv_s[4 * t + zz] = kv_a[j]
        kv_s[4 * (1 - t) + zz] = kv_b[j]
    attend_shard((x + step) % 4, kv_s, q_s, m_s, l_s, acc_s)
    lam_h = jnp.where(z // 4 == t, lam_a[z % 4], lam_b[z % 4])
    gain_row = gain[...] * HEAD_SCALE

    @pl.loop(0, NZ)
    def _(zq):
        denominator = l_s[zq]
        scaled = acc_s[zq] / denominator
        head = scaled[:, 0:HALF] - lam_h * scaled[:, HALF:256]
        square = jnp.mean(head * head, axis=0, keepdims=True)
        head = head * lax.rsqrt(square + EPSILON)
        out[zq, 0:HALF, :] = (head.T * gain_row).astype(BF)
        logs = m_s[zq] * LN2 + jnp.log(denominator)
        high = logs.astype(BF).astype(F32)
        rest = logs - high
        tail = jnp.concatenate(
            [
                high[:, 0:HALF],
                high[:, HALF:256],
                rest[:, 0:HALF],
                rest[:, HALF:256],
                jnp.zeros((4, HALF), F32),
            ],
            axis=0,
        )
        out[zq, HALF : HALF + 8, :] = tail.astype(BF)


STATE = [
    jax.ShapeDtypeStruct((NZ, 1, 256), F32),
    jax.ShapeDtypeStruct((NZ, 1, 256), F32),
    jax.ShapeDtypeStruct((NZ, 128, 256), F32),
]
HELD_STATE = [
    pltpu.VMEM((NZ, 1, 256), F32),
    pltpu.VMEM((NZ, 1, 256), F32),
    pltpu.VMEM((NZ, 128, 256), F32),
]
QUERIES = (NZ, 256, 256)
ATTEND_COST = pl.CostEstimate(
    flops=2 * 36 * BLOCK * 256 * 256, transcendentals=36 * BLOCK * 256, bytes_accessed=4 * 2**20
)


def dma(*shape):
    return pltpu.SemaphoreType.DMA(shape)


def attend_first(q_own, q_peer, kv_a, kv_b):
    return pl.pallas_call(
        first_kernel,
        in_specs=[ANY] * 4,
        out_specs=[ANY] * 4,
        out_shape=[jax.ShapeDtypeStruct(QUERIES, BF)] + STATE,
        scratch_shapes=[pltpu.VMEM((2, 4, 128, HALF), BF), pltpu.VMEM(QUERIES, BF)]
        + HELD_STATE
        + [pltpu.VMEM((NZ, BLOCK, 256), BF), dma(8), dma(NZ), dma(4)],
        cost_estimate=ATTEND_COST,
        name="attend_first",
    )(q_own, q_peer, kv_a, kv_b)


def attend_middle(q_s, state, kv, steps):
    return pl.pallas_call(
        functools.partial(middle_kernel, steps=steps),
        in_specs=[ANY] * 8,
        out_specs=[ANY] * 3,
        out_shape=STATE,
        scratch_shapes=[pltpu.VMEM(QUERIES, BF)]
        + HELD_STATE
        + [pltpu.VMEM((2, NZ, BLOCK, 256), BF), dma(2, 8), dma(NZ), dma(4)],
        cost_estimate=ATTEND_COST,
        name="attend_middle",
    )(q_s, *state, *kv)


def attend_last(lam_a, lam_b, gain, q_s, state, kv_a, kv_b, step):
    return pl.pallas_call(
        functools.partial(last_kernel, step=step),
        in_specs=[SMEM] * 2 + [VMEM] * 7,
        out_specs=VMEM,
        out_shape=jax.ShapeDtypeStruct((NZ, HALF + 8, 128), BF),
        scratch_shapes=HELD_STATE + [pltpu.VMEM((NZ, BLOCK, 256), BF)],
        cost_estimate=ATTEND_COST,
        name="attend_last",
    )(lam_a, lam_b, gain, q_s, *state, kv_a, kv_b)


def weight_copies(ws, held, sems):
    order = [i for d in range(4) for i in (d, 4 + d)]
    return [pltpu.make_async_copy(ws[i], held.at[i], sems.at[i]) for i in order]


def waited(ws, held, sems, d):
    for i in (d, 4 + d):
        pltpu.make_async_copy(ws[0], held.at[i], sems.at[i]).wait()


def conv_mix_kernel(c_own, c_peer, *refs):
    ws, out, held, sems = refs[:8], refs[8], refs[9], refs[10]
    start(weight_copies(ws, held, sems))

    @pl.loop(0, 4)
    def _(d):
        waited(ws, held, sems, d)
        out[d] = jnp.dot(c_own[...], held[d], preferred_element_type=F32) + jnp.dot(
            c_peer[...], held[4 + d], preferred_element_type=F32
        )


def final_kernel(heads, part, *refs):
    ws, out, held, sides, sems = refs[:8], refs[8], refs[9], refs[10], refs[11]
    y, t = lax.axis_index("fs"), lax.axis_index("tp")
    start(weight_copies(ws, held, sems))
    for side, base in ((0, 4 * t), (1, 4 * (1 - t))):
        for i in range(4):
            sides[side, :, i * VD : (i + 1) * VD] = heads[base + i, 0:HALF, :]

    @pl.loop(0, 4)
    def _(d):
        waited(ws, held, sems, d)
        mixed = (
            part[d]
            + jnp.dot(sides[0], held[d], preferred_element_type=F32)
            + jnp.dot(sides[1], held[4 + d], preferred_element_type=F32)
        )
        column = ((y + 4 - d) % 4) * 512
        out[:, pl.ds(pl.multiple_of(column, 512), 512)] = mixed.astype(BF)


MIX_COST = pl.CostEstimate(
    flops=2 * HALF * 1024 * 2048, transcendentals=0, bytes_accessed=6 * 2**20
)
MIX_WEIGHTS = pltpu.VMEM((8, 512, 512), BF)


def conv_mix(c_own, c_peer, ws):
    return pl.pallas_call(
        conv_mix_kernel,
        in_specs=[VMEM] * 2 + [ANY] * 8,
        out_specs=VMEM,
        out_shape=jax.ShapeDtypeStruct((4, HALF, 512), F32),
        scratch_shapes=[MIX_WEIGHTS, dma(8)],
        cost_estimate=MIX_COST,
        name="conv_mix",
    )(c_own, c_peer, *ws)


def final_mix(heads, part, ws):
    return pl.pallas_call(
        final_kernel,
        in_specs=[VMEM] * 2 + [ANY] * 8,
        out_specs=VMEM,
        out_shape=jax.ShapeDtypeStruct((HALF, D), BF),
        scratch_shapes=[MIX_WEIGHTS, pltpu.VMEM((2, HALF, 512), BF), dma(8)],
        cost_estimate=MIX_COST,
        name="final_mix",
    )(heads, part, *ws)


def body(
    inputs,
    norm_gain,
    w_glu_value,
    w_glu_gate,
    w_query_one,
    w_query_two,
    w_key_one,
    w_key_two,
    w_value,
    conv_kernel,
    conv_gain,
    head_gain,
    lambda_head,
    w_out_conv,
    w_out_attn,
):
    return layer(
        inputs,
        norm_gain,
        w_glu_value,
        w_glu_gate,
        (w_key_one, w_key_two, w_query_one, w_query_two, w_value),
        conv_kernel,
        conv_gain,
        head_gain,
        lambda_head,
        w_out_conv,
        w_out_attn,
    )


def swap(value):
    return lax.ppermute(value, "tp", SWAP)


def layer(
    inputs,
    norm_gain,
    w_glu_value,
    w_glu_gate,
    w_qkv,
    conv_kernel,
    conv_gain,
    head_gain,
    lambda_head,
    w_out_conv,
    w_out_attn,
):
    t = lax.axis_index("tp")

    own = inputs[0]
    peer = swap(own)
    normed, *messages = project(own, peer, norm_gain[None], *w_qkv)

    arrived = [lax.ppermute(m, ("z", "tp"), head_route(j)) for j, m in enumerate(messages)]
    kv = jnp.stack([m[:, 0:256] for m in arrived])
    queries = jnp.stack([m[:, 256:384] for m in arrived]).reshape(4, 2, HALF, 128)
    q_own = lax.dynamic_index_in_dim(queries, t, 1, keepdims=False)
    q_peer = swap(lax.dynamic_index_in_dim(queries, 1 - t, 1, keepdims=False))

    shards, swapped = {0: kv}, {0: swap(kv)}
    for step in (1, 3, 2):
        place = (-step) % 4
        shards[place] = lax.ppermute(kv, "x", ring(NX, step))
        swapped[place] = swap(shards[place])

    def gather_weight(w, far_step):
        near = {d: lax.ppermute(w, "fs", ring(NF, d)) for d in (1, 3)}
        far = lax.ppermute(near[far_step], "fs", ring(NF, far_step))
        sides = (w, near[1], far, near[3])
        return sides + tuple(swap(v) for v in sides)

    ws_conv = gather_weight(w_out_conv, 1)
    ws_attn = gather_weight(w_out_attn, 3)
    lambda_peer = swap(lambda_head)

    glu_value = jnp.dot(normed, w_glu_value, preferred_element_type=F32).astype(BF)
    glu_gate = jnp.dot(normed, w_glu_gate, preferred_element_type=F32).astype(BF)
    gated = (glu_value.astype(F32) * jax.nn.sigmoid(glu_gate.astype(F32))).astype(BF)
    count = NZ * NX
    earlier = lax.ppermute(
        gated[BLOCK - (CW - 1) :], ("z", "x"), [(i, i + 1) for i in range(count - 1)]
    )
    extended = jnp.concatenate([earlier, gated], axis=0).astype(F32)
    kernel_f = conv_kernel.astype(F32)
    convolved = jnp.zeros((BLOCK, 512), F32)
    for tap in range(CW):
        convolved = convolved + kernel_f[tap][None, :] * extended[tap : tap + BLOCK]
    sums = jnp.stack([jnp.sum(convolved, axis=-1), jnp.sum(convolved * convolved, axis=-1)])
    sums = sums + swap(sums)
    row_mean = (sums[0] / DC)[:, None]
    row_square = (sums[1] / DC)[:, None]
    conv_out = jax.nn.silu(
        (convolved - row_mean)
        * lax.rsqrt(row_square - row_mean * row_mean + EPSILON)
        * conv_gain
    ).astype(BF)
    conv_halves = conv_out.reshape(2, HALF, 512)
    conv_own = lax.dynamic_index_in_dim(conv_halves, t, 0, keepdims=False)
    conv_other = lax.dynamic_index_in_dim(conv_halves, 1 - t, 0, keepdims=False)
    conv_peer = swap(conv_other)
    part = conv_mix(conv_own, conv_peer, ws_conv)

    q_s, *state = attend_first(q_own, q_peer, shards[0], swapped[0])
    state = attend_middle(
        q_s, state, (shards[3], swapped[3], shards[1], swapped[1]), (3, 1)
    )
    returned = attend_last(
        lambda_head, lambda_peer, head_gain[None], q_s, state, shards[2], swapped[2], 2
    )

    heads = lax.all_to_all(returned, "z", 0, 0, tiled=True)
    mixed = final_mix(heads, part, ws_attn)

    tails = heads[:, HALF : HALF + 4, :].astype(F32)
    logs = (tails[:, 0:2] + tails[:, 2:4]).reshape(2, 4, 2, HALF)
    logs_own = lax.dynamic_index_in_dim(logs, t, 0, keepdims=False)
    logs_peer = swap(lax.dynamic_index_in_dim(logs, 1 - t, 0, keepdims=False))
    first = jnp.where(t == 0, logs_own, logs_peer)
    second = jnp.where(t == 0, logs_peer, logs_own)
    log_sums = jnp.transpose(jnp.concatenate([first, second], axis=-1), (1, 0, 2))
    return (mixed[None], log_sums[None])


def solution(mesh):
    grid = Mesh(mesh.devices.reshape(NZ, NX, NF, NT), ("z", "x", "fs", "tp"))
    weight = P(None, "tp")
    return jax.shard_map(
        body,
        mesh=grid,
        in_specs=(
            P("fs", ("z", "x", "tp"), None),
            P(),
            weight,
            weight,
            weight,
            weight,
            weight,
            weight,
            weight,
            weight,
            P("tp"),
            P(),
            P("tp"),
            P("tp", "fs"),
            P("tp", "fs"),
        ),
        out_specs=(P("fs", ("z", "x", "tp"), None), P("fs", None, "tp", ("z", "x"))),
        check_vma=False,
    )
```

```python
import functools

import jax
import jax.numpy as jnp
from jax import lax
from jax.experimental import pallas as pl
from jax.experimental.pallas import tpu as pltpu
from jax.sharding import Mesh, PartitionSpec as P


D = 2048
DC = 1024
HD = 64
VD = 128
CW = 31
SEG = 64
NZ, NX, NF, NT = 8, 4, 4, 2
BLOCK = 256
HALF = 128

NEG_FILL = -1e30
EPSILON = 1e-05
HEAD_SCALE = 0.8
LOG2E = 1.4426950408889634
LN2 = 0.6931471805599453


SWAP = [(0, 1), (1, 0)]
BF = jnp.bfloat16
F32 = jnp.float32


def head_route(step):
    return [
        (z * NT + t, (4 * t + (z + step) % 4) * NT + z // 4) for z in range(NZ) for t in range(NT)
    ]


def ring(count, step):
    return [(i, (i + step) % count) for i in range(count)]


def proj_kernel(
    own, peer, gain, wk1, wk2, wq1, wq2, wv, x_out, m0, m1, m2, m3, hk1, hk2, hq1, hq2, hv, packed, sems
):
    z, _, t = places()
    copies = [
        pltpu.make_async_copy(w, held, sems.at[i])
        for i, (w, held) in enumerate(
            ((wk1, hk1), (wk2, hk2), (wv, hv), (wq1, hq1), (wq2, hq2))
        )
    ]
    for copy in copies:
        copy.start()
    for place, rows in ((t, own), (1 - t, peer)):
        r = rows[...].astype(F32)
        scale = lax.rsqrt(jnp.mean(r * r, axis=-1, keepdims=True) + EPSILON)
        x_out[pl.ds(pl.multiple_of(place * HALF, HALF), HALF), :] = (r * scale * gain[...]).astype(
            BF
        )
    low = lax.broadcasted_iota(jnp.int32, (BLOCK, 2 * HD), 1) < HD

    def dot(held):
        return jnp.dot(x_out[...], held[...], preferred_element_type=F32).astype(BF).astype(F32)

    def both(a, b, head):
        pair = (head // 2) * 128
        a, b = a[:, pair : pair + 128], b[:, pair : pair + 128]
        if head % 2 == 0:
            return jnp.where(low, a, pltpu.roll(b, HD, 1))
        return jnp.where(low, pltpu.roll(a, HD, 1), b)

    def turned(value, head, column):
        for half in range(2):
            sl = slice(half * HALF, (half + 1) * HALF)
            packed[head, sl, column : column + 128] = value[sl].T.astype(BF)

    copies[0].wait()
    k1 = dot(hk1)
    copies[1].wait()
    k2 = dot(hk2)
    for head in range(4):
        packed[head, :, 0:128] = both(k1, k2, head).astype(BF)
    copies[2].wait()
    v = dot(hv)
    for head in range(4):
        turned(v[:, head * VD : (head + 1) * VD], head, 128)
    copies[3].wait()
    q1 = dot(hq1)
    copies[4].wait()
    q2 = dot(hq2)
    for head in range(4):
        turned(both(q1, q2, head) * (HD**-0.5), head, 256)
    for j, out in enumerate((m0, m1, m2, m3)):
        out[...] = packed[(z + j) % 4]


def project(own, peer, gain, wk1, wk2, wq1, wq2, wv):
    return pl.pallas_call(
        proj_kernel,
        in_specs=[VMEM] * 3 + [ANY] * 5,
        out_specs=[VMEM] * 5,
        out_shape=[jax.ShapeDtypeStruct((BLOCK, D), BF)]
        + [jax.ShapeDtypeStruct((BLOCK, 384), BF)] * 4,
        scratch_shapes=[pltpu.VMEM((D, 256), BF)] * 4
        + [
            pltpu.VMEM((D, 512), BF),
            pltpu.VMEM((4, BLOCK, 384), BF),
            pltpu.SemaphoreType.DMA((5,)),
        ],
        cost_estimate=pl.CostEstimate(
            flops=2 * BLOCK * D * 1536, transcendentals=0, bytes_accessed=8 * 2**20
        ),
        name="project",
    )(own, peer, gain, wk1, wk2, wq1, wq2, wv)


SMEM = pl.BlockSpec(memory_space=pltpu.SMEM)
VMEM = pl.BlockSpec(memory_space=pltpu.VMEM)
ANY = pl.BlockSpec(memory_space=pl.ANY)


def unpack_kernel(m0, m1, m2, m3, kv, q_own, q_other, held, in_sems, sems):
    t = lax.axis_index("tp")
    arrivals = [
        pltpu.make_async_copy(m, held.at[j], in_sems.at[j]) for j, m in enumerate((m0, m1, m2, m3))
    ]
    start(arrivals)
    copies = []
    for j in range(4):
        arrivals[j].wait()
        mine = [pltpu.make_async_copy(held.at[j, :, pl.ds(0, 256)], kv.at[j], sems.at[j])]
        for k, half, q in ((1, t, q_own), (2, 1 - t, q_other)):
            rows = pl.ds(pl.multiple_of(half * HALF, HALF), HALF)
            mine.append(
                pltpu.make_async_copy(
                    held.at[j, rows, pl.ds(256, 128)], q.at[j], sems.at[4 * k + j]
                )
            )
        start(mine)
        copies += mine
    wait(copies)


def unpack(arrived):
    half = jax.ShapeDtypeStruct((4, HALF, 128), BF)
    return pl.pallas_call(
        unpack_kernel,
        in_specs=[ANY] * 4,
        out_specs=[ANY] * 3,
        out_shape=[jax.ShapeDtypeStruct((4, BLOCK, 256), BF), half, half],
        scratch_shapes=[pltpu.VMEM((4, BLOCK, 384), BF), dma(4), dma(12)],
        name="unpack",
    )(*arrived)


def join_kernel(a, b, out, held, in_sems, sems):
    inward = [
        pltpu.make_async_copy(w, held.at[i], in_sems.at[i]) for i, w in enumerate((a, b))
    ]
    outward = [
        pltpu.make_async_copy(held.at[i], out.at[pl.ds(512 * i, 512), :], sems.at[i])
        for i in range(2)
    ]
    start(inward)
    for i in range(2):
        inward[i].wait()
        outward[i].start()
    wait(outward)


def join(a, b):
    return pl.pallas_call(
        join_kernel,
        in_specs=[ANY] * 2,
        out_specs=ANY,
        out_shape=jax.ShapeDtypeStruct((1024, 512), BF),
        scratch_shapes=[pltpu.VMEM((2, 512, 512), BF), dma(2), dma(2)],
        name="join",
    )(a, b)


def places():
    return tuple(lax.axis_index(a) for a in ("z", "x", "tp"))


def shard_copies(kv_a, kv_b, kv_s, sems, first=0):
    z, _, t = places()
    copies = []
    for j in range(kv_a.shape[0]):
        zz = (z + 4 - first - j) % 4
        for slot, kv in ((4 * t + zz, kv_a), (4 * (1 - t) + zz, kv_b)):
            sem = sems.at[2 * (first + j) + (kv is kv_b)]
            copies.append(pltpu.make_async_copy(kv.at[j], kv_s.at[slot], sem))
    return copies


def start(copies):
    for copy in copies:
        copy.start()


def wait(copies):
    for copy in copies:
        copy.wait()


def attend_shard(x2, kv_s, q_s, m_s, l_s, acc_s, before=None, after=None):
    _, x, t = places()
    key_seg = lax.broadcasted_iota(jnp.int32, (BLOCK, 256), 0) // SEG
    query_seg = (lax.broadcasted_iota(jnp.int32, (BLOCK, 256), 1) % HALF) // SEG
    allowed = key_seg - query_seg <= 2 * t + 8 * (x - x2)

    ones = jnp.ones((8, BLOCK), BF)

    def scores(zq):
        q = q_s[zq]
        parts = []
        for z2 in range(zq + 1):
            k = kv_s[z2, :, 0:128]
            s = jnp.dot(jnp.concatenate([k, k], axis=1), q, preferred_element_type=F32)
            if z2 == zq:
                s = jnp.where(allowed, s, NEG_FILL)
            parts.append(s)
        return parts

    def absorb(zq, parts):
        m_old = m_s[zq]
        top = None
        for s in parts:
            best = jnp.max(s.reshape(BLOCK // 8, 8, 256), axis=0)
            top = best if top is None else jnp.maximum(top, best)
        m_new = jnp.maximum(m_old, jnp.max(top, axis=0, keepdims=True))
        factor = jnp.exp2(m_old - m_new)
        weights = []
        values = []
        for z2, s in enumerate(parts):
            weights.append(jnp.exp2(s - m_new).astype(BF))
            vt = jnp.concatenate([kv_s[z2, 0:128, 128:256], kv_s[z2, 128:256, 128:256]], axis=1)
            values.append(jnp.concatenate([vt, ones], axis=0))
        pooled = jnp.dot(
            jnp.concatenate(values, axis=1),
            jnp.concatenate(weights, axis=0),
            preferred_element_type=F32,
        )
        m_s[zq] = m_new
        l_s[zq] = l_s[zq] * factor + pooled[128:129]
        acc_s[zq] = acc_s[zq] * factor + pooled[0:128]

    parts = scores(0)
    if before is not None:
        before()
    for zq in range(NZ):
        following = scores(zq + 1) if zq + 1 < NZ else None
        absorb(zq, parts)
        if after is not None:
            after(zq)
        parts = following


def state_copies(state, held, sems, inward):
    pairs = zip(state, held)
    return [
        pltpu.make_async_copy(*((a, b) if inward else (b, a)), sems.at[i])
        for i, (a, b) in enumerate(pairs)
    ]


def chunk_copy(acc_s, acc, sems, zq):
    return pltpu.make_async_copy(acc_s.at[zq], acc.at[zq], sems.at[zq])


def first_kernel(
    q_own, q_peer, kv_a, kv_b, q_out, m_out, l_out, acc_out, qt_s, q_s, m_s, l_s, acc_s, kv_s, sems, out_sems, aux
):
    z, x, t = places()
    queries = [
        pltpu.make_async_copy(q_own, qt_s.at[0], aux.at[0]),
        pltpu.make_async_copy(q_peer, qt_s.at[1], aux.at[1]),
    ]
    shard = shard_copies(kv_a, kv_b, kv_s, sems)
    start(queries)
    start(shard)
    m_s[...] = jnp.full(m_s.shape, NEG_FILL, F32)
    l_s[...] = jnp.zeros(l_s.shape, F32)
    acc_s[...] = jnp.zeros(acc_s.shape, F32)
    wait(queries)
    upper = lax.broadcasted_iota(jnp.int32, (128, HALF), 0) < HD
    for j in range(4):
        zz = (z + 4 - j) % 4
        for side, base in ((0, 4 * t), (1, 4 * (1 - t))):
            qt = qt_s[side, j].astype(F32) * LOG2E
            high = qt.astype(BF).astype(F32)
            for row, part in ((0, high), (128, qt - high)):
                q_s[base + zz, row : row + 128, 0:HALF] = jnp.where(upper, part, 0.0).astype(BF)
                q_s[base + zz, row : row + 128, HALF:256] = jnp.where(upper, 0.0, part).astype(BF)
    spread = pltpu.make_async_copy(q_s, q_out, aux.at[2])
    spread.start()
    wait(shard)
    chunks = [chunk_copy(acc_s, acc_out, out_sems, zq) for zq in range(NZ)]
    attend_shard(x, kv_s, q_s, m_s, l_s, acc_s, after=lambda zq: chunks[zq].start())
    ends = state_copies((m_out, l_out), (m_s, l_s), aux, False)
    start(ends)
    spread.wait()
    wait(chunks)
    wait(ends)


def middle_kernel(
    q_i,
    m_i,
    l_i,
    acc_i,
    kv_a,
    kv_b,
    kv_c,
    kv_d,
    m_out,
    l_out,
    acc_out,
    q_s,
    m_s,
    l_s,
    acc_s,
    kv_s,
    sems,
    out_sems,
    aux,
    *,
    steps,
):
    _, x, _ = places()
    queries = pltpu.make_async_copy(q_i, q_s, aux.at[3])
    first = shard_copies(kv_a, kv_b, kv_s.at[0], sems.at[0])
    state = state_copies((m_i, l_i, acc_i), (m_s, l_s, acc_s), aux, True)
    second = shard_copies(kv_c, kv_d, kv_s.at[1], sems.at[1])
    queries.start()
    start(first)
    start(state)
    start(second)
    queries.wait()
    wait(first)
    chunks = [chunk_copy(acc_s, acc_out, out_sems, zq) for zq in range(NZ)]

    @pl.loop(0, 2)
    def _(i):
        @pl.when(i == 0)
        def _():
            wait(state)

        @pl.when(i == 1)
        def _():
            wait(second)

        def after(zq):
            @pl.when(i == 1)
            def _():
                chunks[zq].start()

        x2 = (x + jnp.where(i == 0, steps[0], steps[1])) % 4
        attend_shard(x2, kv_s.at[i], q_s, m_s, l_s, acc_s, after=after)

    ends = state_copies((m_out, l_out), (m_s, l_s), aux, False)
    start(ends)
    wait(chunks)
    wait(ends)


def last_kernel(
    lam_a, lam_b, gain, q_s, m_i, l_i, acc_i, kv_a, kv_b, out, m_s, l_s, acc_s, kv_s, *, step
):
    z, x, t = places()
    m_s[...] = m_i[...]
    l_s[...] = l_i[...]
    acc_s[...] = acc_i[...]
    for j in range(4):
        zz = (z + 4 - j) % 4
        kv_s[4 * t + zz] = kv_a[j]
        kv_s[4 * (1 - t) + zz] = kv_b[j]
    attend_shard((x + step) % 4, kv_s, q_s, m_s, l_s, acc_s)
    lam_h = jnp.where(z // 4 == t, lam_a[z % 4], lam_b[z % 4])
    gain_row = gain[...] * HEAD_SCALE

    @pl.loop(0, NZ, unroll=8)
    def _(zq):
        denominator = l_s[zq]
        scaled = acc_s[zq] / denominator
        head = scaled[:, 0:HALF] - lam_h * scaled[:, HALF:256]
        square = jnp.mean(head * head, axis=0, keepdims=True)
        head = head * lax.rsqrt(square + EPSILON)
        out[zq, 0:HALF, :] = (head.T * gain_row).astype(BF)
        logs = m_s[zq] * LN2 + jnp.log(denominator)
        high = logs.astype(BF).astype(F32)
        rest = logs - high
        tail = jnp.concatenate(
            [
                high[:, 0:HALF],
                high[:, HALF:256],
                rest[:, 0:HALF],
                rest[:, HALF:256],
                jnp.zeros((4, HALF), F32),
            ],
            axis=0,
        )
        out[zq, HALF : HALF + 8, :] = tail.astype(BF)


STATE = [
    jax.ShapeDtypeStruct((NZ, 1, 256), F32),
    jax.ShapeDtypeStruct((NZ, 1, 256), F32),
    jax.ShapeDtypeStruct((NZ, 128, 256), F32),
]
HELD_STATE = [
    pltpu.VMEM((NZ, 1, 256), F32),
    pltpu.VMEM((NZ, 1, 256), F32),
    pltpu.VMEM((NZ, 128, 256), F32),
]
QUERIES = (NZ, 256, 256)
ATTEND_COST = pl.CostEstimate(
    flops=2 * 36 * BLOCK * 256 * 256, transcendentals=36 * BLOCK * 256, bytes_accessed=4 * 2**20
)


def dma(*shape):
    return pltpu.SemaphoreType.DMA(shape)


def attend_first(q_own, q_peer, kv_a, kv_b):
    return pl.pallas_call(
        first_kernel,
        in_specs=[ANY] * 4,
        out_specs=[ANY] * 4,
        out_shape=[jax.ShapeDtypeStruct(QUERIES, BF)] + STATE,
        scratch_shapes=[pltpu.VMEM((2, 4, 128, HALF), BF), pltpu.VMEM(QUERIES, BF)]
        + HELD_STATE
        + [pltpu.VMEM((NZ, BLOCK, 256), BF), dma(8), dma(NZ), dma(4)],
        cost_estimate=ATTEND_COST,
        name="attend_first",
    )(q_own, q_peer, kv_a, kv_b)


def attend_middle(q_s, state, kv, steps):
    return pl.pallas_call(
        functools.partial(middle_kernel, steps=steps),
        in_specs=[ANY] * 8,
        out_specs=[ANY] * 3,
        out_shape=STATE,
        scratch_shapes=[pltpu.VMEM(QUERIES, BF)]
        + HELD_STATE
        + [pltpu.VMEM((2, NZ, BLOCK, 256), BF), dma(2, 8), dma(NZ), dma(4)],
        cost_estimate=ATTEND_COST,
        name="attend_middle",
    )(q_s, *state, *kv)


def attend_last(lam_a, lam_b, gain, q_s, state, kv_a, kv_b, step):
    return pl.pallas_call(
        functools.partial(last_kernel, step=step),
        in_specs=[SMEM] * 2 + [VMEM] * 7,
        out_specs=VMEM,
        out_shape=jax.ShapeDtypeStruct((NZ, HALF + 8, 128), BF),
        scratch_shapes=HELD_STATE + [pltpu.VMEM((NZ, BLOCK, 256), BF)],
        cost_estimate=ATTEND_COST,
        name="attend_last",
    )(lam_a, lam_b, gain, q_s, *state, kv_a, kv_b)


def weight_copies(ws, held, sems, first):
    order = [i for d in range(4) for i in (d, 4 + d)]
    rows = pl.ds(first, 512)
    return [pltpu.make_async_copy(ws[i].at[rows, :], held.at[i], sems.at[i]) for i in order]


def waited(ws, held, sems, d):
    for i in (d, 4 + d):
        pltpu.make_async_copy(ws[0].at[pl.ds(0, 512), :], held.at[i], sems.at[i]).wait()


def conv_mix_kernel(c_own, c_peer, *refs):
    ws, out, held, sems = refs[:8], refs[8], refs[9], refs[10]
    start(weight_copies(ws, held, sems, 0))

    @pl.loop(0, 4)
    def _(d):
        waited(ws, held, sems, d)
        out[d] = jnp.dot(c_own[...], held[d], preferred_element_type=F32) + jnp.dot(
            c_peer[...], held[4 + d], preferred_element_type=F32
        )


def final_kernel(heads, part_i, *refs):
    ws = refs[:8]
    out, held, sides, part, out_s, sems, in_sems, out_sems = refs[8:]
    y, t = lax.axis_index("fs"), lax.axis_index("tp")
    rows = [
        pltpu.make_async_copy(
            heads.at[base + i, pl.ds(0, HALF), :],
            sides.at[side, :, pl.ds(i * VD, VD)],
            in_sems.at[4 * side + i],
        )
        for side, base in ((0, 4 * t), (1, 4 * (1 - t)))
        for i in range(4)
    ]
    rows.append(pltpu.make_async_copy(part_i, part, in_sems.at[8]))
    start(rows)
    start(weight_copies(ws, held, sems, 512))
    wait(rows)

    def column(d):
        return pl.ds(pl.multiple_of(((y + 4 - d) % 4) * 512, 512), 512)

    def send(d):
        return pltpu.make_async_copy(
            out_s.at[:, column(d)], out.at[:, column(d)], out_sems.at[d]
        )

    @pl.loop(0, 4)
    def _(d):
        waited(ws, held, sems, d)
        mixed = (
            part[d]
            + jnp.dot(sides[0], held[d], preferred_element_type=F32)
            + jnp.dot(sides[1], held[4 + d], preferred_element_type=F32)
        )
        out_s[:, column(d)] = mixed.astype(BF)
        send(d).start()

    for d in range(4):
        send(d).wait()


MIX_COST = pl.CostEstimate(
    flops=2 * HALF * 1024 * 2048, transcendentals=0, bytes_accessed=6 * 2**20
)
MIX_WEIGHTS = pltpu.VMEM((8, 512, 512), BF)


def conv_mix(c_own, c_peer, ws):
    return pl.pallas_call(
        conv_mix_kernel,
        in_specs=[VMEM] * 2 + [ANY] * 8,
        out_specs=VMEM,
        out_shape=jax.ShapeDtypeStruct((4, HALF, 512), F32),
        scratch_shapes=[MIX_WEIGHTS, dma(8)],
        cost_estimate=MIX_COST,
        name="conv_mix",
    )(c_own, c_peer, *ws)


def final_mix(heads, part, ws):
    return pl.pallas_call(
        final_kernel,
        in_specs=[ANY] * 10,
        out_specs=ANY,
        out_shape=jax.ShapeDtypeStruct((HALF, D), BF),
        scratch_shapes=[
            MIX_WEIGHTS,
            pltpu.VMEM((2, HALF, 512), BF),
            pltpu.VMEM((4, HALF, 512), F32),
            pltpu.VMEM((HALF, D), BF),
            dma(8),
            dma(9),
            dma(4),
        ],
        cost_estimate=MIX_COST,
        name="final_mix",
    )(heads, part, *ws)


def body(
    inputs,
    norm_gain,
    w_glu_value,
    w_glu_gate,
    w_query_one,
    w_query_two,
    w_key_one,
    w_key_two,
    w_value,
    conv_kernel,
    conv_gain,
    head_gain,
    lambda_head,
    w_out_conv,
    w_out_attn,
):
    return layer(
        inputs,
        norm_gain,
        w_glu_value,
        w_glu_gate,
        (w_key_one, w_key_two, w_query_one, w_query_two, w_value),
        conv_kernel,
        conv_gain,
        head_gain,
        lambda_head,
        w_out_conv,
        w_out_attn,
    )


def swap(value):
    return lax.ppermute(value, "tp", SWAP)


def layer(
    inputs,
    norm_gain,
    w_glu_value,
    w_glu_gate,
    w_qkv,
    conv_kernel,
    conv_gain,
    head_gain,
    lambda_head,
    w_out_conv,
    w_out_attn,
):
    t = lax.axis_index("tp")

    own = inputs[0]
    peer = swap(own)
    normed, *messages = project(own, peer, norm_gain[None], *w_qkv)

    arrived = [lax.ppermute(m, ("z", "tp"), head_route(j)) for j, m in enumerate(messages)]
    kv, q_own, q_other = unpack(arrived)
    q_peer = swap(q_other)

    shards, swapped = {0: kv}, {0: swap(kv)}
    for step in (1, 3, 2):
        place = (-step) % 4
        shards[place] = lax.ppermute(kv, "x", ring(NX, step))
        swapped[place] = swap(shards[place])

    w_own = join(w_out_conv, w_out_attn)
    w_sides = [w_own] + [lax.ppermute(w_own, "fs", ring(NF, d)) for d in (1, 2, 3)]
    w_all = w_sides + [swap(w) for w in w_sides]
    lambda_peer = swap(lambda_head)

    glu_value = jnp.dot(normed, w_glu_value, preferred_element_type=F32).astype(BF)
    glu_gate = jnp.dot(normed, w_glu_gate, preferred_element_type=F32).astype(BF)
    gated = (glu_value.astype(F32) * jax.nn.sigmoid(glu_gate.astype(F32))).astype(BF)
    count = NZ * NX
    earlier = lax.ppermute(
        gated[BLOCK - (CW - 1) :], ("z", "x"), [(i, i + 1) for i in range(count - 1)]
    )
    extended = jnp.concatenate([earlier, gated], axis=0).astype(F32)
    kernel_f = conv_kernel.astype(F32)
    convolved = jnp.zeros((BLOCK, 512), F32)
    for tap in range(CW):
        convolved = convolved + kernel_f[tap][None, :] * extended[tap : tap + BLOCK]
    sums = jnp.stack([jnp.sum(convolved, axis=-1), jnp.sum(convolved * convolved, axis=-1)])
    sums = sums + swap(sums)
    row_mean = (sums[0] / DC)[:, None]
    row_square = (sums[1] / DC)[:, None]
    conv_out = jax.nn.silu(
        (convolved - row_mean)
        * lax.rsqrt(row_square - row_mean * row_mean + EPSILON)
        * conv_gain
    ).astype(BF)
    conv_halves = conv_out.reshape(2, HALF, 512)
    conv_own = lax.dynamic_index_in_dim(conv_halves, t, 0, keepdims=False)
    conv_other = lax.dynamic_index_in_dim(conv_halves, 1 - t, 0, keepdims=False)
    conv_peer = swap(conv_other)
    part = conv_mix(conv_own, conv_peer, w_all)

    q_s, *state = attend_first(q_own, q_peer, shards[0], swapped[0])
    state = attend_middle(
        q_s, state, (shards[3], swapped[3], shards[1], swapped[1]), (3, 1)
    )
    returned = attend_last(
        lambda_head, lambda_peer, head_gain[None], q_s, state, shards[2], swapped[2], 2
    )

    heads = lax.all_to_all(returned, "z", 0, 0, tiled=True)
    heads, part = lax.optimization_barrier((heads, part))
    mixed = final_mix(heads, part, w_all)

    tails = heads[:, HALF : HALF + 4, :].astype(F32)
    logs = (tails[:, 0:2] + tails[:, 2:4]).reshape(2, 4, 2, HALF)
    logs_own = lax.dynamic_index_in_dim(logs, t, 0, keepdims=False)
    logs_peer = swap(lax.dynamic_index_in_dim(logs, 1 - t, 0, keepdims=False))
    first = jnp.where(t == 0, logs_own, logs_peer)
    second = jnp.where(t == 0, logs_peer, logs_own)
    log_sums = jnp.transpose(jnp.concatenate([first, second], axis=-1), (1, 0, 2))
    return (mixed[None], log_sums[None])


def solution(mesh):
    grid = Mesh(mesh.devices.reshape(NZ, NX, NF, NT), ("z", "x", "fs", "tp"))
    weight = P(None, "tp")
    return jax.shard_map(
        body,
        mesh=grid,
        in_specs=(
            P("fs", ("z", "x", "tp"), None),
            P(),
            weight,
            weight,
            weight,
            weight,
            weight,
            weight,
            weight,
            weight,
            P("tp"),
            P(),
            P("tp"),
            P("tp", "fs"),
            P("tp", "fs"),
        ),
        out_specs=(P("fs", ("z", "x", "tp"), None), P("fs", None, "tp", ("z", "x"))),
        check_vma=False,
    )
```
